128 devices in a mesh: fs: 16 (over z, x), tp: 8 (over y, core).
Axes of the slice: x: 4, y: 4, z: 4, core: 2. Of those that a mesh axis runs over, the one named last changes fastest.
Arguments:
- prompts: bfloat16 [8, 1024, 2048], P('tp'), may hold values from -6 to 6
- gain_first: float32 [2048], P('fs'), may hold values from 0.1 to 1.9
- gate_first: float32 [2048, 5632], P('fs', 'tp'), may hold values from -0.125 to 0.125
- up_first: float32 [2048, 5632], P('fs', 'tp'), may hold values from -0.125 to 0.125
- down_first: float32 [5632, 2048], P('fs', 'tp'), may hold values from -0.078125 to 0.078125
- gain_second: float32 [2048], P('fs'), may hold values from 0.1 to 1.9
- gate_second: float32 [2048, 5632], P('fs', 'tp'), may hold values from -0.125 to 0.125
- up_second: float32 [2048, 5632], P('fs', 'tp'), may hold values from -0.125 to 0.125
- down_second: float32 [5632, 2048], P('fs', 'tp'), may hold values from -0.078125 to 0.078125
Outputs:
- served_gate_first: bfloat16 [2048, 5632], P(None, 'fs')
- served_up_first: bfloat16 [2048, 5632], P(None, 'fs')
- served_down_first: bfloat16 [5632, 2048], P('fs')
- served_gate_second: bfloat16 [2048, 5632], P(None, 'fs')
- served_up_second: bfloat16 [2048, 5632], P(None, 'fs')
- served_down_second: bfloat16 [5632, 2048], P('fs')
- prompt_states: bfloat16 [8, 1024, 2048], P('tp', 'fs')
The draws below stay inside these ranges and needn't reach their ends.
All inputs are finite; a program needn't handle non-finite values.
Results may differ from the reference program's by a relative error of at most 0.012.
Values may be sent and summed in bfloat16 or wider, within the bound.
No kernel may reach another device: no remote copies, remote signals or barrier semaphores. Data moves between devices by JAX's collectives and lax.ppermute only.
A program may use at most 128 MiB of HBM per device.

```python
import jax
import jax.numpy as jnp
from jax import lax

D = 2048
FF = 5632
PLEN = 1024
PROMPTS = 8
N_FS = 16


def levels(rng, dims, cuts, smallest, top_value):
    gain, own = 1.0, jax.random.fold_in(rng, 6)
    for dim, parts in cuts:
        draws = jnp.exp(jax.random.uniform(jax.random.fold_in(own, dim), (parts,), jnp.float32, smallest / len(cuts), top_value / len(cuts)))
        gain = gain * jnp.repeat(draws, dims[dim] // parts).reshape([-1 if axis == dim else 1 for axis in range(len(dims))])
    return gain


def bell_draw(own_key, dims, spread, bound, split=(), held_as=jnp.bfloat16):
    factor_of = levels(own_key, dims, split, -0.22, 0.18) if split else 1.0
    result = jax.random.normal(own_key, dims, jnp.float32) * spread * factor_of
    return jnp.minimum(jnp.maximum(result, -bound), bound).astype(held_as)


def setup_inputs(seed: int = 0) -> dict:
    splits = jax.random.split(jax.random.key(seed), 10)
    prompts = bell_draw(splits[0], (PROMPTS, PLEN, D), 1.0, 6.0, ((0, 8),))
    gain_first = jnp.clip(1.0 + 0.18 * jax.random.normal(splits[1], (D,), jnp.float32), 0.1, 1.9)
    gate_first = bell_draw(splits[2], (D, FF), D ** -0.5, 0.125, ((0, 16), (1, 8)), jnp.float32)
    up_first = bell_draw(splits[3], (D, FF), D ** -0.5, 0.125, ((0, 16), (1, 8)), jnp.float32)
    down_first = bell_draw(splits[4], (FF, D), FF ** -0.5, 0.078125, ((0, 16), (1, 8)), jnp.float32)
    gain_second = jnp.clip(1.0 + 0.18 * jax.random.normal(splits[5], (D,), jnp.float32), 0.1, 1.9)
    gate_second = bell_draw(splits[6], (D, FF), D ** -0.5, 0.125, ((0, 16), (1, 8)), jnp.float32)
    up_second = bell_draw(splits[7], (D, FF), D ** -0.5, 0.125, ((0, 16), (1, 8)), jnp.float32)
    down_second = bell_draw(splits[8], (FF, D), FF ** -0.5, 0.078125, ((0, 16), (1, 8)), jnp.float32)
    return dict(prompts=prompts, gain_first=gain_first, gate_first=gate_first, up_first=up_first, down_first=down_first, gain_second=gain_second, gate_second=gate_second, up_second=up_second, down_second=down_second)


def normalize(row_block):
    widened = row_block.astype(jnp.float32)
    scaled = widened * lax.rsqrt(lax.optimization_barrier(jnp.mean(widened * widened, axis=-1, keepdims=True)) + 1e-06)
    return scaled.astype(jnp.bfloat16)

def block_sum(active, down_rows):
    unit_count = active.shape[1] // N_FS

    def advance(running, block_index):
        left_cols = lax.dynamic_slice_in_dim(active, block_index * unit_count, unit_count, 1)
        right_rows = lax.dynamic_slice_in_dim(down_rows, block_index * unit_count, unit_count, 0)
        partial_sum = jnp.dot(left_cols, right_rows, preferred_element_type=jnp.float32).astype(jnp.bfloat16)
        partial_sum = lax.optimization_barrier(partial_sum)
        return (running + partial_sum.astype(jnp.float32), None)
    start_sum = jnp.zeros((active.shape[0], down_rows.shape[1]), jnp.float32)
    running, _ = lax.scan(advance, start_sum, jnp.arange(N_FS, dtype=jnp.int32))
    return running

def half_step(tokens_in, gate_cols, up_cols, down_rows):
    normed = normalize(tokens_in)
    gate_val = jnp.dot(normed, gate_cols, preferred_element_type=jnp.float32)
    up_val = jnp.dot(normed, up_cols, preferred_element_type=jnp.float32)
    active = (jax.nn.silu(gate_val) * up_val).astype(jnp.bfloat16)
    branch = block_sum(active, down_rows)
    return (tokens_in.astype(jnp.float32) + 0.5 * branch).astype(jnp.bfloat16)

def reference(prompts, gain_first, gate_first, up_first, down_first, gain_second, gate_second, up_second, down_second):
    served_gate_first = (gain_first[:, None] * gate_first).astype(jnp.bfloat16)
    served_up_first = (gain_first[:, None] * up_first).astype(jnp.bfloat16)
    served_gate_second = (gain_second[:, None] * gate_second).astype(jnp.bfloat16)
    served_up_second = (gain_second[:, None] * up_second).astype(jnp.bfloat16)
    served_down_first = down_first.astype(jnp.bfloat16)
    served_down_second = down_second.astype(jnp.bfloat16)
    tokens_in = prompts.reshape(-1, prompts.shape[-1])
    middle = half_step(tokens_in, served_gate_first, served_up_first, served_down_first)
    finished = half_step(middle, served_gate_second, served_up_second, served_down_second)
    return (served_gate_first, served_up_first, served_down_first, served_gate_second, served_up_second, served_down_second, finished.reshape(prompts.shape))
```

```python
import jax
import jax.numpy as jnp
from jax import lax
from jax.sharding import Mesh
from jax.sharding import PartitionSpec as P


FS = ("z", "x")
TP = ("y", "core")
ALL = ("z", "x", "y", "core")
BF = jnp.bfloat16
F32 = jnp.float32


def shift(value, axis, by):
    n = lax.axis_size(axis)
    return lax.ppermute(value, axis, [(i, (i + by) % n) for i in range(n)])


def paired(value, axis, partner):
    n = lax.axis_size(axis)
    return lax.ppermute(value, axis, [(i, partner(i)) for i in range(n)])


def to_server(k):
    def flat(z, x, y, c):
        return ((z * 4 + x) * 4 + y) * 2 + c

    return [
        (flat(z, x, y, c), flat(y, 2 * c + ((x % 2) ^ k), z, x // 2))
        for z in range(4)
        for x in range(4)
        for y in range(4)
        for c in range(2)
    ]


def folded(gain, trained):
    return (gain[:, None] * trained).astype(BF).T


def serve_rows(gain, gate, up):
    g, u = folded(gain, gate), folded(gain, up)
    half = g.shape[0] // 2
    low = jnp.concatenate([g[:half], u[:half]], axis=0)
    high = jnp.concatenate([g[half:], u[half:]], axis=0)
    odd = (lax.axis_index("x") & 1) == 1
    first = lax.ppermute(jnp.where(odd, high, low), ALL, to_server(0))
    second = lax.ppermute(jnp.where(odd, low, high), ALL, to_server(1))
    return jnp.concatenate(
        [jnp.where(odd, second, first), jnp.where(odd, first, second)], axis=1
    )


def from_y(piece):
    return [piece, shift(piece, "y", -1), shift(piece, "y", -2), shift(piece, "y", 1)]


def in_order(same):
    other = paired(same, "core", lambda i: 1 - i)
    both = jnp.concatenate([same, other], axis=0)
    y, c = lax.axis_index("y"), lax.axis_index("core")
    cols = []
    for t in range(8):
        at = ((t // 2 - y) & 3) + 4 * ((t % 2) ^ c)
        cols.append(lax.dynamic_index_in_dim(both, at, 0, keepdims=False))
    return jnp.concatenate(cols, axis=1)


def normalize(row_block):
    widened = row_block.astype(F32)
    scaled = widened * lax.rsqrt(jnp.mean(widened * widened, axis=-1, keepdims=True) + 1e-06)
    return scaled.astype(BF)


def dot_t(a, b_t):
    return lax.dot_general(a, b_t, (((1,), (1,)), ((), ())), preferred_element_type=F32)


def partial_branch(tokens, weights):
    unit = weights.shape[0] // 3
    normed = normalize(tokens)
    gate_val = dot_t(normed, weights[:unit])
    up_val = dot_t(normed, weights[unit : 2 * unit])
    active = (jax.nn.silu(gate_val) * up_val).astype(BF)
    return jnp.dot(active, weights[2 * unit :], preferred_element_type=F32).astype(BF)


def wide_sum(*terms):
    total = terms[0].astype(F32)
    for t in terms[1:]:
        total = total + t.astype(F32)
    return total


def per_device(
    prompts,
    gain_first,
    gate_first,
    up_first,
    down_first,
    gain_second,
    gate_second,
    up_second,
    down_second,
):
    z, x = lax.axis_index("z"), lax.axis_index("x")
    width = prompts.shape[-1]

    down_rows = from_y(down_first.astype(BF))
    gate_up = from_y(serve_rows(gain_first, gate_first, up_first))
    weights_a = in_order(
        jnp.stack([jnp.concatenate([gu, dn], axis=0) for gu, dn in zip(gate_up, down_rows)])
    )

    tokens = prompts.reshape(4, 4, 2, 32, width)
    half_a = tokens[:, :, 0]
    half_b = tokens[:, :, 1].transpose(1, 0, 2, 3)
    group_a = [
        lax.dynamic_index_in_dim(half_a, (z + r) & 3, 0, keepdims=False).reshape(128, width)
        for r in range(4)
    ]
    group_b = [
        lax.dynamic_index_in_dim(half_b, (x + r) & 3, 0, keepdims=False).reshape(128, width)
        for r in range(4)
    ]

    gu_b = serve_rows(gain_second, gate_second, up_second)
    piece_b = jnp.concatenate([gu_b, down_second.astype(BF)], axis=0)
    weights_b = in_order(jnp.stack(from_y(piece_b)))

    def exchanged(groups, weights):
        got_a, got_b = [None] * 4, [None] * 4
        for r in (2, 1, 3, 0):
            part = partial_branch(groups[r], weights)
            if r:
                got_a[r] = shift(part[:128], "z", r)
                got_b[r] = shift(part[128:], "x", r)
            else:
                got_a[0], got_b[0] = part[:128], part[128:]
        return wide_sum(*got_a), wide_sum(*got_b)

    groups = [jnp.concatenate([a, b], axis=0) for a, b in zip(group_a, group_b)]
    sum_a, sum_b = exchanged(groups, weights_a)

    near = lambda i: i ^ 1
    far = lambda i: 3 - i
    s_a, s_b = sum_a.astype(BF), sum_b.astype(BF)
    a0, a1, b0, b1 = s_a[:64], s_a[64:], s_b[:64], s_b[64:]
    a0, a1, b0, b1 = (
        wide_sum(a0, paired(a0, "x", near)).astype(BF),
        wide_sum(a1, paired(a1, "x", far)).astype(BF),
        wide_sum(b0, paired(b0, "z", near)).astype(BF),
        wide_sum(b1, paired(b1, "z", far)).astype(BF),
    )
    a0, a1, b0, b1 = (
        wide_sum(a0, paired(a0, "x", far)),
        wide_sum(a1, paired(a1, "x", near)),
        wide_sum(b0, paired(b0, "z", far)),
        wide_sum(b1, paired(b1, "z", near)),
    )
    branch_a = jnp.concatenate([a0, a1], axis=0)
    branch_b = jnp.concatenate([b0, b1], axis=0)
    mid_a = (group_a[0].astype(F32) + 0.5 * branch_a).astype(BF)
    mid_b = (group_b[0].astype(F32) + 0.5 * branch_b).astype(BF)

    middle = [jnp.concatenate([mid_a, mid_b], axis=0)]
    for r in (1, 2, 3):
        middle.append(jnp.concatenate([shift(mid_a, "z", -r), shift(mid_b, "x", -r)], axis=0))

    end_a, end_b = exchanged(middle, weights_b)
    e_a = end_a.astype(BF).reshape(4, 32, width)
    e_b = end_b.astype(BF).reshape(4, 32, width)
    own_a = [lax.dynamic_index_in_dim(e_a, (x + r) & 3, 0, keepdims=False) for r in range(4)]
    own_b = [lax.dynamic_index_in_dim(e_b, (z + r) & 3, 0, keepdims=False) for r in range(4)]
    fin_a = wide_sum(own_a[0], *[shift(own_a[r], "x", r) for r in (1, 2, 3)])
    fin_b = wide_sum(own_b[0], *[shift(own_b[r], "z", r) for r in (1, 2, 3)])
    m_a = lax.dynamic_index_in_dim(mid_a.reshape(4, 32, width), x, 0, keepdims=False)
    m_b = lax.dynamic_index_in_dim(mid_b.reshape(4, 32, width), z, 0, keepdims=False)
    finished = jnp.concatenate(
        [
            (m_a.astype(F32) + 0.5 * fin_a).astype(BF),
            (m_b.astype(F32) + 0.5 * fin_b).astype(BF),
        ],
        axis=0,
    )[None]

    unit = weights_a.shape[0] // 3
    outs = []
    for w in (weights_a, weights_b):
        outs += [w[:unit].T, w[unit : 2 * unit].T, w[2 * unit :]]
    return (*outs, finished)


def solution(mesh):
    split = Mesh(mesh.devices.reshape(4, 4, 4, 2), ALL)
    placed = (
        P(TP, None, None),
        P(FS),
        P(FS, TP),
        P(FS, TP),
        P(FS, TP),
        P(FS),
        P(FS, TP),
        P(FS, TP),
        P(FS, TP),
    )
    return jax.shard_map(
        per_device,
        mesh=split,
        in_specs=placed,
        out_specs=(
            P(None, FS),
            P(None, FS),
            P(FS, None),
            P(None, FS),
            P(None, FS),
            P(FS, None),
            P(TP, FS, None),
        ),
        check_vma=False,
    )
```
